32 devices in a mesh: ep: 8 (over z, x), tp: 4 (over y, core).
Axes of the slice: x: 2, y: 2, z: 4, core: 2. Of those that a mesh axis runs over, the one named last changes fastest.
Arguments:
- tokens: bfloat16 [64, 4096], P('ep', 'tp'), may hold values from -6 to 6
- norm_gain: float32 [4096], replicated, may hold values from 0.1 to 1.9
- route_experts: int32 [64, 2], P('ep'), may hold values from 0 to 15, all different within a row; in each aligned block of 8 rows (0 to 7, 8 to 15, ...) at most 2 rows name the same one
- route_logits: float32 [64, 2], P('ep'), may hold values from -4 to 4
- expert_gate: bfloat16 [16, 4096, 1024], P('ep', None, 'tp'), may hold values from -0.09375 to 0.09375
- expert_up: bfloat16 [16, 4096, 1024], P('ep', None, 'tp'), may hold values from -0.09375 to 0.09375
- expert_down: bfloat16 [16, 1024, 4096], P('ep', 'tp'), may hold values from -0.1875 to 0.1875
- dense_gate: bfloat16 [4096, 1024], P(None, 'tp'), may hold values from -0.09375 to 0.09375
- dense_up: bfloat16 [4096, 1024], P(None, 'tp'), may hold values from -0.09375 to 0.09375
- dense_down: bfloat16 [1024, 4096], P('tp'), may hold values from -0.1875 to 0.1875
- mix_weight: float32 [4096], replicated, may hold values from -0.09375 to 0.09375
- out_gain: float32 [4096], P('tp'), may hold values from 0.1 to 1.9
Outputs:
- result: bfloat16 [64, 4096], P('ep', 'tp')
The draws below stay inside these ranges and needn't reach their ends.
Inputs may be any that keep to these rules, and one draw needn't show every extreme that they name: `route_experts`: each row names 2 different experts; the 8 rows of one index of ep (aligned blocks) name any one expert at most 2 times, and some block names some expert exactly 2 times; every expert is named somewhere.
All inputs are finite; a program needn't handle non-finite values.
Results may differ from the reference program's by a relative error of at most 0.0025.
Values may be sent and summed in bfloat16 or wider, within the bound.
A program may use at most 64 MiB of HBM per device.

```python
import math
import jax
import jax.numpy as jnp
import numpy as np
from jax import lax

D = 4096
FFE = 1024
DENSE_FF = 1024
TOP = 2
CAP = 2
TOK_DEV = 8
EXPERTS = 16
TOKENS = 64
N_EP = 8


def levels(rng, dims, pieces, low, high):
    level = 1.0
    for dim, shards_of in pieces:
        draws = jax.random.uniform(jax.random.fold_in(jax.random.fold_in(rng, 6), dim), (shards_of,), jnp.float32, low / len(pieces), high / len(pieces))
        level = level * jnp.repeat(jnp.exp(draws), dims[dim] // shards_of).reshape((-1,) + (1,) * (len(dims) - 1 - dim))
    return level


def shared_out(key, own, number, rows, amount, top, reach, lean):
    sequence = jax.random.permutation(key, amount)
    crowded, usual = load_shares(amount, rows * top, reach, lean, True), load_shares(amount, rows * top, reach, lean, False)
    places = jnp.arange(amount)

    def named(tallies, offset_by):
        used = int((tallies > 0).sum())
        fixed = max(1, used // 4)
        shifted = fixed + (places - fixed + offset_by * (used - fixed)) % max(1, amount - fixed)
        return jnp.zeros((amount,), jnp.int32).at[sequence[jnp.where(places < fixed, places, shifted)]].set(jnp.asarray(tallies, jnp.int32))

    tallies = jnp.where(number % 4 == 0, named(crowded, number // 4), named(usual, number - number // 4 - 1))
    mixed = jax.random.permutation(jax.random.fold_in(own, 3), amount)
    donor, taker = mixed[0:amount // 2 * 2:2], mixed[1:amount // 2 * 2:2]
    margin = jnp.minimum(tallies[donor] - 1, reach - tallies[taker]) // 2
    margin = jnp.where((donor == sequence[0]) | (taker == sequence[0]) | (tallies[taker] == 0), 0, jnp.maximum(margin, 0))
    shifted = jax.random.randint(jax.random.fold_in(own, 4), (amount // 2,), 0, 1 << 20) % (margin + 1)
    tallies = tallies.at[donor].add(-shifted).at[taker].add(shifted)
    items = jnp.searchsorted(jnp.cumsum(tallies), jnp.arange(rows * top), side="right").astype(jnp.int32)
    table = items.reshape(top, rows).T
    table = table[jax.random.permutation(jax.random.fold_in(own, 1), rows)]
    offset_by = jax.random.randint(jax.random.fold_in(own, 2), (rows, 1), 0, top)
    return jnp.take_along_axis(table, (jnp.arange(top)[None, :] + offset_by) % top, axis=1)


def load_shares(number_of, total, reach, slope, full):
    loads = [(1 << 20) // math.isqrt(grade ** slope) + 1 for grade in range(1, number_of + 1)]
    largest = reach if full else min(reach, max(-(-total // number_of), total * loads[0] // sum(loads)))
    least = 1 if total - largest >= number_of - 1 else 0
    holding, surplus = [largest] + [least] * (number_of - 1), total - largest - least * (number_of - 1)
    while surplus > 0:
        free = [i for i in range(1, number_of) if holding[i] < largest] or [i for i in range(1, number_of) if holding[i] < reach]
        mass, remaining = sum([loads[i] for i in free]), surplus
        for i in free:
            addition = min(reach - holding[i], max(1, remaining * loads[i] // mass), surplus)
            holding[i] = holding[i] + addition
            surplus = surplus - addition
    return np.array(holding)


def centred(rng, dims, scale, limit, shards=(), held_as=jnp.bfloat16):
    result = jax.random.normal(rng, dims, jnp.float32) * scale
    if len(shards) > 0:
        result = levels(rng, dims, shards, -0.22, 0.18) * result
    return jnp.clip(result, min=-limit, max=limit).astype(held_as)


def setup_inputs(seed: int = 0) -> dict:
    seeds = jax.random.split(jax.random.key(seed), 13)
    tokens = centred(seeds[0], (TOKENS, D), 1.0, 6.0, ((0, 8), (1, 4)))
    norm_gain = jnp.clip(1.0 + 0.18 * jax.random.normal(seeds[1], (D,), jnp.float32), 0.1, 1.9)
    route_experts_keys = jax.random.split(jax.random.fold_in(seeds[2], 1), TOKENS // TOK_DEV)
    route_experts_turns = jax.random.permutation(jax.random.fold_in(seeds[2], 3), TOKENS // TOK_DEV)
    route_experts = jax.vmap(lambda own, number: shared_out(jax.random.fold_in(seeds[2], 2), own, number, TOK_DEV, EXPERTS, TOP, CAP, 2))(route_experts_keys, route_experts_turns).reshape((TOKENS, TOP))
    route_logits = centred(seeds[3], (TOKENS, TOP), 1.0, 4.0, ((0, 8),), jnp.float32)
    expert_gate = centred(seeds[4], (EXPERTS, D, FFE), D ** -0.5, 0.09375, ((0, 8), (2, 4)))
    expert_up = centred(seeds[5], (EXPERTS, D, FFE), D ** -0.5, 0.09375, ((0, 8), (2, 4)))
    expert_down = centred(seeds[6], (EXPERTS, FFE, D), FFE ** -0.5, 0.1875, ((0, 8), (1, 4)))
    dense_gate = centred(seeds[7], (D, DENSE_FF), D ** -0.5, 0.09375, ((1, 4),))
    dense_up = centred(seeds[8], (D, DENSE_FF), D ** -0.5, 0.09375, ((1, 4),))
    dense_down = centred(seeds[9], (DENSE_FF, D), DENSE_FF ** -0.5, 0.1875, ((0, 4),))
    mix_weight = centred(seeds[10], (D,), D ** -0.5, 0.09375, (), jnp.float32)
    out_gain = jnp.clip(1.0 + 0.18 * jax.random.normal(seeds[11], (D,), jnp.float32), 0.1, 1.9)
    return dict(tokens=tokens, norm_gain=norm_gain, route_experts=route_experts, route_logits=route_logits, expert_gate=expert_gate, expert_up=expert_up, expert_down=expert_down, dense_gate=dense_gate, dense_up=dense_up, dense_down=dense_down, mix_weight=mix_weight, out_gain=out_gain)


norm_eps = 1e-06

def reference(tokens, norm_gain, route_experts, route_logits, expert_gate, expert_up, expert_down, dense_gate, dense_up, dense_down, mix_weight, out_gain):
    values = tokens.astype(jnp.float32)
    normed = (values * lax.rsqrt(lax.optimization_barrier(jnp.mean(values * values, axis=1, keepdims=True)) + norm_eps) * norm_gain).astype(jnp.bfloat16)
    weights = jax.nn.softmax(route_logits, axis=-1)
    rows_cap = N_EP * CAP

    def per_expert(running, expert):
        route_hits = route_experts == expert
        routed = jnp.any(route_hits, axis=1)
        row_index = jnp.nonzero(routed, size=rows_cap, fill_value=0)[0].astype(jnp.int32)
        row_count = jnp.sum(routed.astype(jnp.int32))
        usable = (jnp.arange(rows_cap, dtype=jnp.int32) < row_count).astype(jnp.float32)
        picked = normed[row_index]
        gate_act = jnp.dot(picked, expert_gate[expert], preferred_element_type=jnp.float32)
        up_act = jnp.dot(picked, expert_up[expert], preferred_element_type=jnp.float32)
        hidden = (jax.nn.silu(gate_act) * up_act).astype(jnp.bfloat16)
        produced = jnp.dot(hidden, expert_down[expert], preferred_element_type=jnp.float32)
        factor = lax.optimization_barrier(jnp.sum(jnp.where(route_hits, weights, jnp.zeros_like(weights)), axis=1))[row_index] * usable
        return (running.at[row_index].add(factor[:, None] * produced), None)
    expert_mix, _ = lax.scan(per_expert, jnp.zeros((TOKENS, D), jnp.float32), jnp.arange(EXPERTS, dtype=jnp.int32))
    dense_hidden = (jax.nn.silu(jnp.dot(normed, dense_gate, preferred_element_type=jnp.float32)) * jnp.dot(normed, dense_up, preferred_element_type=jnp.float32)).astype(jnp.bfloat16)
    dense_out = jnp.dot(dense_hidden, dense_down, preferred_element_type=jnp.float32)
    mix_gate = jax.nn.sigmoid(jnp.dot(normed.astype(jnp.float32), mix_weight, precision=lax.Precision.HIGHEST))
    combined = expert_mix + mix_gate[:, None] * dense_out
    scaled = combined * lax.rsqrt(lax.optimization_barrier(jnp.mean(combined * combined, axis=1, keepdims=True)) + norm_eps) * out_gain
    return scaled.astype(jnp.bfloat16)
```

```python
import functools

import jax
import jax.numpy as jnp
from jax import lax
from jax.experimental import pallas as pl
from jax.experimental.pallas import tpu as pltpu
from jax.sharding import PartitionSpec as P

CAP = 2
CORES = 2
norm_eps = 1e-06
MESH = pl.DeviceIdType.MESH
F32 = jnp.float32
BF16 = jnp.bfloat16


def silu(v):
    return v / (1.0 + jnp.exp(-v))


def kernel(
    n_ep,
    n_tp,
    tok_hbm,
    gain_hbm,
    route_hbm,
    logit_hbm,
    eg_hbm,
    eu_hbm,
    ed_hbm,
    dg_hbm,
    du_hbm,
    dd_hbm,
    mix_hbm,
    og_hbm,
    out_ref,
    tok,
    gain,
    route,
    logit,
    eg,
    eu,
    ed,
    dg,
    du,
    dd,
    mixw,
    og,
    normed,
    placed,
    disp_send,
    disp_recv,
    rows_f,
    dense_send,
    dense_recv,
    pair_send,
    pair_recv,
    summed,
    ret_send,
    ret_recv,
    back,
    sq_send,
    sq_recv,
    lsem,
    ag_s,
    ag_r,
    di_s,
    di_r,
    fw_s,
    fw_r,
    de_s,
    de_r,
    pa_s,
    pa_r,
    re_s,
    re_r,
    sq_s,
    sq_r,
):
    me = lax.axis_index("ep")
    tp = lax.axis_index("tp")
    core = lax.rem(tp, CORES)
    row = lax.div(tp, CORES)
    n_row = n_tp // CORES
    partner = row * CORES + (1 - core)
    n_loc = eg.shape[0]
    t_rows, part = tok.shape[1], tok.shape[2]
    width = part * n_tp
    half = width // CORES
    blk = n_loc * CAP
    slots = n_ep * blk

    def turn(base, d, n):
        return lax.rem(base + d, n)

    def remote(src, dst, s, r, e, t):
        return pltpu.make_async_remote_copy(
            src_ref=src,
            dst_ref=dst,
            send_sem=s,
            recv_sem=r,
            device_id={"ep": e, "tp": t},
            device_id_type=MESH,
        )

    loads = []
    pairs = [
        (tok_hbm, tok.at[tp]),
        (gain_hbm, gain),
        (route_hbm, route),
        (logit_hbm, logit),
        (mix_hbm, mixw),
        (og_hbm, og),
        (dg_hbm, dg),
        (du_hbm, du),
        (dd_hbm, dd),
        (eg_hbm, eg),
        (eu_hbm, eu),
        (ed_hbm, ed),
    ]
    for i, (src, dst) in enumerate(pairs):
        c = pltpu.make_async_copy(src, dst, lsem.at[i])
        c.start()
        loads.append(c)

    barrier = pltpu.get_barrier_semaphore()
    greeted = 0
    for d in range(1, n_ep):
        for y in range(n_row):
            pl.semaphore_signal(
                barrier,
                inc=1,
                device_id={"ep": turn(me, d, n_ep), "tp": y * CORES + core},
                device_id_type=MESH,
            )
            greeted += 1
    for d in range(1, n_tp):
        pl.semaphore_signal(
            barrier, inc=1, device_id={"ep": me, "tp": turn(tp, d, n_tp)}, device_id_type=MESH
        )
        greeted += 1
    pl.semaphore_wait(barrier, greeted)

    loads[0].wait()
    gathers = []
    for d in range(1, n_tp):
        c = remote(tok.at[tp], tok.at[tp], ag_s.at[d], ag_r.at[d], me, turn(tp, d, n_tp))
        c.start()
        gathers.append(c)

    for i in range(1, 6):
        loads[i].wait()
    r0 = route[:, 0:1]
    r1 = route[:, 1:2]
    l0 = logit[:, 0:1]
    l1 = logit[:, 1:2]
    top = jnp.maximum(l0, l1)
    e0 = jnp.exp(l0 - top)
    e1 = jnp.exp(l1 - top)
    w0 = e0 / (e0 + e1)
    w1 = e1 / (e0 + e1)
    slot_e = lax.broadcasted_iota(jnp.int32, (t_rows, slots), 1) // CAP
    slot_c = lax.broadcasted_iota(jnp.int32, (t_rows, slots), 1) % CAP
    hit0 = (slot_e == r0).astype(F32)
    hit1 = (slot_e == r1).astype(F32)
    hits = hit0 + hit1
    ri = lax.broadcasted_iota(jnp.int32, (t_rows, t_rows), 0)
    ci = lax.broadcasted_iota(jnp.int32, (t_rows, t_rows), 1)
    before = jnp.dot((ci < ri).astype(F32), hits, preferred_element_type=F32)
    place = hits * (before == slot_c.astype(F32)).astype(F32)
    combine = place * (hit0 * w0 + hit1 * w1)
    place_t = place.T.astype(BF16)

    for c in gathers:
        c.wait_recv()
    squares = jnp.zeros((t_rows, 1), F32)
    for t in range(n_tp):
        x = tok[t].astype(F32)
        squares += jnp.sum(x * x, axis=1, keepdims=True)
    inv = lax.rsqrt(squares / width + norm_eps)
    mix = jnp.zeros((t_rows, 1), F32)
    for t in range(n_tp):
        cols = pl.ds(t * part, part)
        nx = (tok[t].astype(F32) * inv * gain[:, cols]).astype(BF16)
        normed[:, cols] = nx
        mix += jnp.sum(nx.astype(F32) * mixw[:, cols], axis=1, keepdims=True)
    mix_gate = 1.0 / (1.0 + jnp.exp(-mix))

    my_half = pl.ds(pl.multiple_of(core * half, 128), half)
    placed[...] = jnp.dot(place_t, normed[:, my_half], preferred_element_type=F32)
    for p in range(n_ep):
        disp_send[p] = placed[p * blk : (p + 1) * blk, :].astype(BF16)
    disp_recv[core, me] = disp_send[me]
    sends = []
    for d in range(1, n_ep):
        p = turn(me, d, n_ep)
        c = remote(disp_send.at[p], disp_recv.at[core, me], di_s.at[d], di_r.at[d], p, tp)
        c.start()
        sends.append(c)

    for i in (6, 7, 8):
        loads[i].wait()
    nrm = normed[...]
    dh = (
        silu(jnp.dot(nrm, dg[...], preferred_element_type=F32))
        * jnp.dot(nrm, du[...], preferred_element_type=F32)
    ).astype(BF16)
    dense = []
    for t in range(n_tp):
        dense_send[t] = jnp.dot(
            dh, dd[:, t * part : (t + 1) * part], preferred_element_type=F32
        )
    for d in range(1, n_tp):
        t = turn(tp, d, n_tp)
        c = remote(dense_send.at[t], dense_recv.at[tp], de_s.at[d], de_r.at[d], me, t)
        c.start()
        dense.append(c)
    dense_recv[tp] = dense_send[tp]

    forwards = []
    for d in range(n_ep):
        q = turn(me, n_ep - d, n_ep)
        if d > 0:
            sends[d - 1].wait_recv()
        c = remote(disp_recv.at[core, q], disp_recv.at[core, q], fw_s.at[d], fw_r.at[d], me, partner)
        c.start()
        forwards.append(c)
    for i in (9, 10, 11):
        loads[i].wait()
    for c in forwards:
        c.wait_recv()
    for h in range(CORES):
        for p in range(n_ep):
            rows_f[p * blk : (p + 1) * blk, h * half : (h + 1) * half] = disp_recv[h, p].astype(F32)
    x = rows_f[...].astype(BF16)
    which = (lax.broadcasted_iota(jnp.int32, (slots, 1), 0) % blk) // CAP
    hidden = []
    for e in range(n_loc):
        h = silu(jnp.dot(x, eg[e], preferred_element_type=F32)) * jnp.dot(
            x, eu[e], preferred_element_type=F32
        )
        hidden.append(jnp.where(which == e, h, 0.0).astype(BF16))

    def down(t):
        cols = pl.ds(pl.multiple_of(t * part, 128), part)
        total = jnp.dot(hidden[0], ed[0, :, cols], preferred_element_type=F32)
        for e in range(1, n_loc):
            total += jnp.dot(hidden[e], ed[e, :, cols], preferred_element_type=F32)
        return total

    duo = []
    for y in range(n_row):
        pair_send[y] = down(y * CORES + (1 - core))
        c = remote(pair_send.at[y], pair_recv.at[y], pa_s.at[y], pa_r.at[y], me, partner)
        c.start()
        duo.append(c)
    for y in range(n_row):
        summed[y] = down(y * CORES + core)
    returns = []
    for y in range(n_row):
        duo[y].wait_recv()
        summed[y] += pair_recv[y]
        for p in range(n_ep):
            ret_send[y, p] = summed[y, p * blk : (p + 1) * blk, :]
    for d in range(1, n_ep):
        p = turn(me, d, n_ep)
        for k in range(n_row):
            y = turn(row, k, n_row)
            i = d * n_row + k
            c = remote(
                ret_send.at[y, p],
                ret_recv.at[row, me],
                re_s.at[i],
                re_r.at[i],
                p,
                y * CORES + core,
            )
            c.start()
            returns.append(c)
    for k in range(1, n_row):
        y = turn(row, k, n_row)
        c = remote(
            ret_send.at[y, me], ret_recv.at[row, me], re_s.at[k], re_r.at[k], me, y * CORES + core
        )
        c.start()
        returns.append(c)
    ret_recv[row, me] = ret_send[row, me]

    for c in dense:
        c.wait_recv()
    total = dense_recv[0]
    for t in range(1, n_tp):
        total += dense_recv[t]
    total = mix_gate * total
    for c in returns:
        c.wait_recv()
    for p in range(n_ep):
        s = ret_recv[0, p]
        for y in range(1, n_row):
            s += ret_recv[y, p]
        back[p * blk : (p + 1) * blk, :] = s
    total += jnp.dot(
        combine, back[...], preferred_element_type=F32, precision=lax.Precision.HIGHEST
    )
    sq_send[...] = jnp.broadcast_to(
        jnp.sum(total * total, axis=1, keepdims=True), sq_send.shape
    )
    swaps = []
    for d in range(1, n_tp):
        c = remote(sq_send, sq_recv.at[tp], sq_s.at[d], sq_r.at[d], me, turn(tp, d, n_tp))
        c.start()
        swaps.append(c)
    sq_recv[tp] = sq_send[...]
    for c in swaps:
        c.wait_recv()
    all_sq = sq_recv[0]
    for t in range(1, n_tp):
        all_sq += sq_recv[t]
    scale = lax.rsqrt(all_sq[:, 0:1] / width + norm_eps)
    out_ref[...] = (total * scale * og[...]).astype(out_ref.dtype)
    for c in gathers + sends + dense + forwards + duo + returns + swaps:
        c.wait_send()


def shards(n_ep, n_tp, *args):
    (tok, gain, route, logit, eg, eu, ed, dg, du, dd, mixw, og) = args
    t_rows, part = tok.shape
    width = part * n_tp
    n_loc, _, ff = eg.shape
    n_row = n_tp // CORES
    half = width // CORES
    blk = n_loc * CAP
    slots = n_ep * blk
    dma = pltpu.SemaphoreType.DMA
    V = pltpu.VMEM
    scratch = [
        V((n_tp, t_rows, part), BF16),
        V((1, width), F32),
        V(route.shape, jnp.int32),
        V(logit.shape, F32),
        V(eg.shape, BF16),
        V(eu.shape, BF16),
        V(ed.shape, BF16),
        V(dg.shape, BF16),
        V(du.shape, BF16),
        V(dd.shape, BF16),
        V((1, width), F32),
        V((1, part), F32),
        V((t_rows, width), BF16),
        V((slots, half), F32),
        V((n_ep, blk, half), BF16),
        V((CORES, n_ep, blk, half), BF16),
        V((slots, width), F32),
        V((n_tp, t_rows, part), F32),
        V((n_tp, t_rows, part), F32),
        V((n_row, slots, part), F32),
        V((n_row, slots, part), F32),
        V((n_row, slots, part), F32),
        V((n_row, n_ep, blk, part), F32),
        V((n_row, n_ep, blk, part), F32),
        V((slots, part), F32),
        V((t_rows, 128), F32),
        V((n_tp, t_rows, 128), F32),
        dma((12,)),
        dma((n_tp,)),
        dma((n_tp,)),
        dma((n_ep,)),
        dma((n_ep,)),
        dma((n_ep,)),
        dma((n_ep,)),
        dma((n_tp,)),
        dma((n_tp,)),
        dma((n_row,)),
        dma((n_row,)),
        dma((n_ep * n_row,)),
        dma((n_ep * n_row,)),
        dma((n_tp,)),
        dma((n_tp,)),
    ]
    return pl.pallas_call(
        functools.partial(kernel, n_ep, n_tp),
        out_shape=jax.ShapeDtypeStruct((t_rows, part), BF16),
        in_specs=[pl.BlockSpec(memory_space=pltpu.HBM)] * 12,
        out_specs=pl.BlockSpec(memory_space=pltpu.VMEM),
        scratch_shapes=scratch,
        compiler_params=pltpu.CompilerParams(
            collective_id=0, has_side_effects=True, vmem_limit_bytes=60 * 1024 * 1024
        ),
        name="moe_layer",
    )(
        tok,
        gain.reshape(1, width),
        route,
        logit,
        eg,
        eu,
        ed,
        dg,
        du,
        dd,
        mixw.reshape(1, width),
        og.reshape(1, part),
    )


def solution(mesh):
    placed = (
        P("ep", "tp"),
        P(),
        P("ep", None),
        P("ep", None),
        P("ep", None, "tp"),
        P("ep", None, "tp"),
        P("ep", "tp", None),
        P(None, "tp"),
        P(None, "tp"),
        P("tp", None),
        P(),
        P("tp"),
    )
    return jax.shard_map(
        functools.partial(shards, mesh.shape["ep"], mesh.shape["tp"]),
        mesh=mesh,
        in_specs=placed,
        out_specs=P("ep", "tp"),
        check_vma=False,
    )
```

```python
import functools

import jax
import jax.numpy as jnp
from jax import lax
from jax.experimental import pallas as pl
from jax.experimental.pallas import tpu as pltpu
from jax.sharding import PartitionSpec as P

CAP = 2
CORES = 2
norm_eps = 1e-06
MESH = pl.DeviceIdType.MESH
F32 = jnp.float32
BF16 = jnp.bfloat16


def silu(v):
    return v / (1.0 + jnp.exp(-v))


def kernel(
    n_ep,
    n_tp,
    tok_hbm,
    gain_hbm,
    route_hbm,
    logit_hbm,
    eg_hbm,
    eu_hbm,
    ed_hbm,
    dg_hbm,
    du_hbm,
    dd_hbm,
    mix_hbm,
    og_hbm,
    out_ref,
    tok,
    gain,
    route,
    logit,
    eg,
    eu,
    ed,
    dg,
    du,
    dd,
    mixw,
    og,
    normed,
    placed,
    disp_send,
    disp_recv,
    rows_f,
    rows_n,
    dense_send,
    dense_recv,
    pair_send,
    pair_recv,
    summed,
    ret_send,
    ret_recv,
    back,
    sq_send,
    sq_recv,
    lsem,
    ag_s,
    ag_r,
    di_s,
    di_r,
    fw_s,
    fw_r,
    de_s,
    de_r,
    pa_s,
    pa_r,
    re_s,
    re_r,
    sq_s,
    sq_r,
):
    me = lax.axis_index("ep")
    tp = lax.axis_index("tp")
    core = lax.rem(tp, CORES)
    row = lax.div(tp, CORES)
    n_row = n_tp // CORES
    partner = row * CORES + (1 - core)
    n_loc = eg.shape[0]
    t_rows, part = tok.shape[1], tok.shape[2]
    width = part * n_tp
    blk = n_loc * CAP
    slots = n_ep * blk

    def turn(base, d, n):
        return lax.rem(base + d, n)

    def remote(src, dst, s, r, e, t):
        return pltpu.make_async_remote_copy(
            src_ref=src,
            dst_ref=dst,
            send_sem=s,
            recv_sem=r,
            device_id={"ep": e, "tp": t},
            device_id_type=MESH,
        )

    loads = []
    pairs = [
        (tok_hbm, tok.at[tp]),
        (gain_hbm, gain),
        (route_hbm, route),
        (logit_hbm, logit),
        (mix_hbm, mixw),
        (og_hbm, og),
        (dg_hbm, dg),
        (du_hbm, du),
        (dd_hbm, dd),
        (eg_hbm, eg),
        (eu_hbm, eu),
        (ed_hbm, ed),
    ]
    for i, (src, dst) in enumerate(pairs):
        c = pltpu.make_async_copy(src, dst, lsem.at[i])
        c.start()
        loads.append(c)

    barrier = pltpu.get_barrier_semaphore()
    greeted = 0
    for d in range(1, n_ep):
        for y in range(n_row):
            pl.semaphore_signal(
                barrier,
                inc=1,
                device_id={"ep": turn(me, d, n_ep), "tp": y * CORES + core},
                device_id_type=MESH,
            )
            greeted += 1
    for d in range(1, n_tp):
        pl.semaphore_signal(
            barrier, inc=1, device_id={"ep": me, "tp": turn(tp, d, n_tp)}, device_id_type=MESH
        )
        greeted += 1
    pl.semaphore_wait(barrier, greeted)

    near = sorted(range(1, n_ep), key=lambda d: min(d, n_ep - d))

    loads[0].wait()
    gathers = []
    for d in range(1, n_tp):
        gathers.append(
            remote(tok.at[tp], tok.at[tp], ag_s.at[d], ag_r.at[d], me, turn(tp, d, n_tp))
        )

    loads[2].wait()
    r0 = route[0:1, :]
    r1 = route[1:2, :]
    slot = lax.broadcasted_iota(jnp.int32, (slots, t_rows), 0)
    slot_e = slot // CAP
    slot_c = slot % CAP
    hit0 = (slot_e == r0).astype(F32)
    hit1 = (slot_e == r1).astype(F32)
    hits = hit0 + hit1
    ri = lax.broadcasted_iota(jnp.int32, (t_rows, t_rows), 0)
    ci = lax.broadcasted_iota(jnp.int32, (t_rows, t_rows), 1)
    before = jnp.dot(hits, (ri < ci).astype(F32), preferred_element_type=F32)
    place_t = hits * (before == slot_c.astype(F32)).astype(F32)

    placed[...] = jnp.dot(place_t.astype(BF16), tok[tp], preferred_element_type=F32)
    for p in range(n_ep):
        disp_send[p] = placed[p * blk : (p + 1) * blk, :].astype(BF16)
    sends = {}
    for d in reversed(near):
        p = turn(me, d, n_ep)
        c = remote(disp_send.at[p], disp_recv.at[tp, me], di_s.at[d], di_r.at[d], p, tp)
        c.start()
        sends[d] = c
    disp_recv[tp, me] = disp_send[me]
    for c in gathers:
        c.start()

    for d in [0] + near:
        q = turn(me, n_ep - d, n_ep)
        if d > 0:
            sends[d].wait_recv()
        for k in range(1, n_tp):
            remote(
                disp_recv.at[tp, q],
                disp_recv.at[tp, q],
                fw_s.at[k],
                fw_r.at[k],
                me,
                turn(tp, k, n_tp),
            ).start()

    for i in (1, 3, 4, 5):
        loads[i].wait()
    l0 = logit[0:1, :]
    l1 = logit[1:2, :]
    top = jnp.maximum(l0, l1)
    e0 = jnp.exp(l0 - top)
    e1 = jnp.exp(l1 - top)
    w0 = e0 / (e0 + e1)
    w1 = e1 / (e0 + e1)
    combine = (place_t * (hit0 * w0 + hit1 * w1)).T

    for c in gathers:
        c.wait_recv()
    squares = jnp.zeros((t_rows, 1), F32)
    for t in range(n_tp):
        x = tok[t].astype(F32)
        squares += jnp.sum(x * x, axis=1, keepdims=True)
    inv = lax.rsqrt(squares / width + norm_eps)
    mix = jnp.zeros((t_rows, 1), F32)
    for t in range(n_tp):
        cols = pl.ds(t * part, part)
        nx = (tok[t].astype(F32) * inv * gain[:, cols]).astype(BF16)
        normed[:, cols] = nx
        mix += jnp.sum(nx.astype(F32) * mixw[:, cols], axis=1, keepdims=True)
    mix_gate = 1.0 / (1.0 + jnp.exp(-mix))

    for i in (6, 7, 8):
        loads[i].wait()
    nrm = normed[...]
    dh = (
        silu(jnp.dot(nrm, dg[...], preferred_element_type=F32))
        * jnp.dot(nrm, du[...], preferred_element_type=F32)
    ).astype(BF16)
    dense = []
    for t in range(n_tp):
        dense_send[t] = jnp.dot(
            dh, dd[:, t * part : (t + 1) * part], preferred_element_type=F32
        )
    for d in range(1, n_tp):
        t = turn(tp, d, n_tp)
        c = remote(dense_send.at[t], dense_recv.at[tp], de_s.at[d], de_r.at[d], me, t)
        c.start()
        dense.append(c)
    dense_recv[tp] = dense_send[tp]

    for i in (9, 10, 11):
        loads[i].wait()
    forwards = []
    for k in range(1, n_tp):
        c = remote(
            disp_recv.at[tp],
            disp_recv.at[turn(tp, n_tp - k, n_tp)],
            fw_s.at[k],
            fw_r.at[k],
            me,
            turn(tp, k, n_tp),
        )
        c.wait_recv()
        forwards.append(c)
    squares = jnp.zeros((slots, 1), F32)
    for t in range(n_tp):
        cols = pl.ds(t * part, part)
        for p in range(n_ep):
            rows_f[p * blk : (p + 1) * blk, cols] = disp_recv[t, p].astype(F32)
        x = rows_f[:, cols]
        squares += jnp.sum(x * x, axis=1, keepdims=True)
    inv = lax.rsqrt(squares / width + norm_eps)
    for t in range(n_tp):
        cols = pl.ds(t * part, part)
        rows_n[:, cols] = (rows_f[:, cols] * inv * gain[:, cols]).astype(BF16)
    x = rows_n[...]
    which = (lax.broadcasted_iota(jnp.int32, (slots, 1), 0) % blk) // CAP
    hidden = []
    for e in range(n_loc):
        h = silu(jnp.dot(x, eg[e], preferred_element_type=F32)) * jnp.dot(
            x, eu[e], preferred_element_type=F32
        )
        hidden.append(jnp.where(which == e, h, 0.0).astype(BF16))

    def down(t):
        cols = pl.ds(pl.multiple_of(t * part, 128), part)
        total = jnp.dot(hidden[0], ed[0, :, cols], preferred_element_type=F32)
        for e in range(1, n_loc):
            total += jnp.dot(hidden[e], ed[e, :, cols], preferred_element_type=F32)
        return total

    duo = []
    for y in range(n_row):
        pair_send[y] = down(y * CORES + (1 - core))
        c = remote(pair_send.at[y], pair_recv.at[y], pa_s.at[y], pa_r.at[y], me, partner)
        c.start()
        duo.append(c)
    for y in range(n_row):
        summed[y] = down(y * CORES + core)
    returns = []
    for y in range(n_row):
        duo[y].wait_recv()
        summed[y] += pair_recv[y]
        for p in range(n_ep):
            ret_send[y, p] = summed[y, p * blk : (p + 1) * blk, :]
    for d in range(1, n_ep):
        p = turn(me, d, n_ep)
        for k in range(n_row):
            y = turn(row, k, n_row)
            i = d * n_row + k
            c = remote(
                ret_send.at[y, p],
                ret_recv.at[row, me],
                re_s.at[i],
                re_r.at[i],
                p,
                y * CORES + core,
            )
            c.start()
            returns.append(c)
    for k in range(1, n_row):
        y = turn(row, k, n_row)
        c = remote(
            ret_send.at[y, me], ret_recv.at[row, me], re_s.at[k], re_r.at[k], me, y * CORES + core
        )
        c.start()
        returns.append(c)
    ret_recv[row, me] = ret_send[row, me]

    for c in dense:
        c.wait_recv()
    total = dense_recv[0]
    for t in range(1, n_tp):
        total += dense_recv[t]
    total = mix_gate * total
    for c in returns:
        c.wait_recv()
    for p in range(n_ep):
        s = ret_recv[0, p]
        for y in range(1, n_row):
            s += ret_recv[y, p]
        back[p * blk : (p + 1) * blk, :] = s
    total += jnp.dot(
        combine, back[...], preferred_element_type=F32, precision=lax.Precision.HIGHEST
    )
    sq_send[...] = jnp.broadcast_to(
        jnp.sum(total * total, axis=1, keepdims=True), sq_send.shape
    )
    swaps = []
    for d in range(1, n_tp):
        c = remote(sq_send, sq_recv.at[tp], sq_s.at[d], sq_r.at[d], me, turn(tp, d, n_tp))
        c.start()
        swaps.append(c)
    sq_recv[tp] = sq_send[...]
    for c in swaps:
        c.wait_recv()
    all_sq = sq_recv[0]
    for t in range(1, n_tp):
        all_sq += sq_recv[t]
    scale = lax.rsqrt(all_sq[:, 0:1] / width + norm_eps)
    out_ref[...] = (total * scale * og[...]).astype(out_ref.dtype)
    for c in gathers + list(sends.values()) + dense + forwards + duo + returns + swaps:
        c.wait_send()


def shards(n_ep, n_tp, *args):
    (tok, gain, route, logit, eg, eu, ed, dg, du, dd, mixw, og) = args
    t_rows, part = tok.shape
    width = part * n_tp
    n_loc, _, ff = eg.shape
    n_row = n_tp // CORES
    blk = n_loc * CAP
    slots = n_ep * blk
    dma = pltpu.SemaphoreType.DMA
    V = pltpu.VMEM
    scratch = [
        V((n_tp, t_rows, part), BF16),
        V((1, width), F32),
        V(route.shape[::-1], jnp.int32),
        V(logit.shape[::-1], F32),
        V(eg.shape, BF16),
        V(eu.shape, BF16),
        V(ed.shape, BF16),
        V(dg.shape, BF16),
        V(du.shape, BF16),
        V(dd.shape, BF16),
        V((1, width), F32),
        V((1, part), F32),
        V((t_rows, width), BF16),
        V((slots, part), F32),
        V((n_ep, blk, part), BF16),
        V((n_tp, n_ep, blk, part), BF16),
        V((slots, width), F32),
        V((slots, width), BF16),
        V((n_tp, t_rows, part), F32),
        V((n_tp, t_rows, part), F32),
        V((n_row, slots, part), F32),
        V((n_row, slots, part), F32),
        V((n_row, slots, part), F32),
        V((n_row, n_ep, blk, part), F32),
        V((n_row, n_ep, blk, part), F32),
        V((slots, part), F32),
        V((t_rows, 128), F32),
        V((n_tp, t_rows, 128), F32),
        dma((12,)),
        dma((n_tp,)),
        dma((n_tp,)),
        dma((n_ep,)),
        dma((n_ep,)),
        dma((n_tp,)),
        dma((n_tp,)),
        dma((n_tp,)),
        dma((n_tp,)),
        dma((n_row,)),
        dma((n_row,)),
        dma((n_ep * n_row,)),
        dma((n_ep * n_row,)),
        dma((n_tp,)),
        dma((n_tp,)),
    ]
    return pl.pallas_call(
        functools.partial(kernel, n_ep, n_tp),
        out_shape=jax.ShapeDtypeStruct((t_rows, part), BF16),
        in_specs=[pl.BlockSpec(memory_space=pltpu.HBM)] * 12,
        out_specs=pl.BlockSpec(memory_space=pltpu.VMEM),
        scratch_shapes=scratch,
        compiler_params=pltpu.CompilerParams(
            collective_id=0, has_side_effects=True, vmem_limit_bytes=60 * 1024 * 1024
        ),
        name="moe_layer",
    )(
        tok,
        gain.reshape(1, width),
        route.T,
        logit.T,
        eg,
        eu,
        ed,
        dg,
        du,
        dd,
        mixw.reshape(1, width),
        og.reshape(1, part),
    )


def solution(mesh):
    placed = (
        P("ep", "tp"),
        P(),
        P("ep", None),
        P("ep", None),
        P("ep", None, "tp"),
        P("ep", None, "tp"),
        P("ep", "tp", None),
        P(None, "tp"),
        P(None, "tp"),
        P("tp", None),
        P(),
        P("tp"),
    )
    return jax.shard_map(
        functools.partial(shards, mesh.shape["ep"], mesh.shape["tp"]),
        mesh=mesh,
        in_specs=placed,
        out_specs=P("ep", "tp"),
        check_vma=False,
    )
```

```python
import functools

import jax
import jax.numpy as jnp
from jax import lax
from jax.experimental import pallas as pl
from jax.experimental.pallas import tpu as pltpu
from jax.sharding import PartitionSpec as P

CAP = 2
CORES = 2
norm_eps = 1e-06
LOG2E = 1.4426950408889634
MESH = pl.DeviceIdType.MESH
F32 = jnp.float32
BF16 = jnp.bfloat16


def silu(v):
    return v / (1.0 + jnp.exp(-v))


def kernel(
    n_ep,
    n_tp,
    tok_hbm,
    gain_hbm,
    route_hbm,
    logit_hbm,
    eg_hbm,
    eu_hbm,
    ed_hbm,
    dg_hbm,
    du_hbm,
    dd_hbm,
    mix_hbm,
    og_hbm,
    out_ref,
    tok,
    gain,
    route,
    logit,
    eg,
    eu,
    ed,
    dg,
    du,
    dd,
    mixw,
    og,
    normed,
    placed,
    disp_send,
    disp_recv,
    rows_f,
    rows_n,
    dense_send,
    dense_recv,
    pair_send,
    pair_recv,
    summed,
    coded,
    ret_send,
    ret_recv,
    back,
    sq_send,
    sq_recv,
    lsem,
    ag_s,
    ag_r,
    di_s,
    di_r,
    fw_s,
    fw_r,
    de_s,
    de_r,
    pa_s,
    pa_r,
    re_s,
    re_r,
    sq_s,
    sq_r,
):
    me = lax.axis_index("ep")
    tp = lax.axis_index("tp")
    core = lax.rem(tp, CORES)
    row = lax.div(tp, CORES)
    n_row = n_tp // CORES
    partner = row * CORES + (1 - core)
    n_loc = eg.shape[0]
    t_rows, part = tok.shape[1], tok.shape[2]
    width = part * n_tp
    blk = n_loc * CAP
    slots = n_ep * blk

    def turn(base, d, n):
        return lax.rem(base + d, n)

    def remote(src, dst, s, r, e, t):
        return pltpu.make_async_remote_copy(
            src_ref=src,
            dst_ref=dst,
            send_sem=s,
            recv_sem=r,
            device_id={"ep": e, "tp": t},
            device_id_type=MESH,
        )

    loads = []
    pairs = [
        (tok_hbm, tok.at[tp]),
        (gain_hbm, gain),
        (route_hbm, route),
        (logit_hbm, logit),
        (mix_hbm, mixw),
        (og_hbm, og),
        (dg_hbm, dg),
        (du_hbm, du),
        (dd_hbm, dd),
        (eg_hbm, eg),
        (eu_hbm, eu),
        (ed_hbm, ed),
    ]
    for i, (src, dst) in enumerate(pairs):
        c = pltpu.make_async_copy(src, dst, lsem.at[i])
        c.start()
        loads.append(c)

    barrier = pltpu.get_barrier_semaphore()
    greeted = 0
    for d in range(1, n_ep):
        for y in range(n_row):
            pl.semaphore_signal(
                barrier,
                inc=1,
                device_id={"ep": turn(me, d, n_ep), "tp": y * CORES + core},
                device_id_type=MESH,
            )
            greeted += 1
    for d in range(1, n_tp):
        pl.semaphore_signal(
            barrier, inc=1, device_id={"ep": me, "tp": turn(tp, d, n_tp)}, device_id_type=MESH
        )
        greeted += 1
    pl.semaphore_wait(barrier, greeted)

    near = sorted(range(1, n_ep), key=lambda d: min(d, n_ep - d))

    loads[0].wait()
    gathers = []
    for d in range(1, n_tp):
        gathers.append(
            remote(tok.at[tp], tok.at[tp], ag_s.at[d], ag_r.at[d], me, turn(tp, d, n_tp))
        )

    loads[2].wait()
    r0 = route[0:1, :]
    r1 = route[1:2, :]
    slot = lax.broadcasted_iota(jnp.int32, (slots, t_rows), 0)
    slot_e = slot // CAP
    slot_c = slot % CAP
    hit0 = (slot_e == r0).astype(F32)
    hit1 = (slot_e == r1).astype(F32)
    hits = hit0 + hit1
    ri = lax.broadcasted_iota(jnp.int32, (t_rows, t_rows), 0)
    ci = lax.broadcasted_iota(jnp.int32, (t_rows, t_rows), 1)
    before = jnp.dot(hits, (ri < ci).astype(F32), preferred_element_type=F32)
    place_t = hits * (before == slot_c.astype(F32)).astype(F32)

    placed[...] = jnp.dot(place_t.astype(BF16), tok[tp], preferred_element_type=F32)
    for p in range(n_ep):
        disp_send[p] = placed[p * blk : (p + 1) * blk, :].astype(BF16)
    sends = {}
    for d in reversed(near):
        p = turn(me, d, n_ep)
        c = remote(disp_send.at[p], disp_recv.at[tp, me], di_s.at[d], di_r.at[d], p, tp)
        c.start()
        sends[d] = c
    disp_recv[tp, me] = disp_send[me]
    for c in gathers:
        c.start()

    for d in [0] + near:
        q = turn(me, n_ep - d, n_ep)
        if d > 0:
            sends[d].wait_recv()
        for k in range(1, n_tp):
            remote(
                disp_recv.at[tp, q],
                disp_recv.at[tp, q],
                fw_s.at[k],
                fw_r.at[k],
                me,
                turn(tp, k, n_tp),
            ).start()

    for i in (1, 3, 4, 5):
        loads[i].wait()
    l0 = logit[0:1, :]
    l1 = logit[1:2, :]
    top = jnp.maximum(l0, l1)
    e0 = jnp.exp(l0 - top)
    e1 = jnp.exp(l1 - top)
    w0 = e0 / (e0 + e1)
    w1 = e1 / (e0 + e1)
    combine = (place_t * (hit0 * w0 + hit1 * w1)).T

    for c in gathers:
        c.wait_recv()
    squares = jnp.zeros((t_rows, 1), F32)
    for t in range(n_tp):
        x = tok[t].astype(F32)
        squares += jnp.sum(x * x, axis=1, keepdims=True)
    inv = lax.rsqrt(squares / width + norm_eps)
    mix = jnp.zeros((t_rows, 1), F32)
    for t in range(n_tp):
        cols = pl.ds(t * part, part)
        nx = (tok[t].astype(F32) * inv * gain[:, cols]).astype(BF16)
        normed[:, cols] = nx
        mix += jnp.sum(nx.astype(F32) * mixw[:, cols], axis=1, keepdims=True)
    mix_gate = 1.0 / (1.0 + jnp.exp(-mix))

    for i in (6, 7, 8):
        loads[i].wait()
    nrm = normed[...]
    dh = (
        silu(jnp.dot(nrm, dg[...], preferred_element_type=F32))
        * jnp.dot(nrm, du[...], preferred_element_type=F32)
    ).astype(BF16)
    dense = []
    for t in range(n_tp):
        dense_send[t] = jnp.dot(
            dh, dd[:, t * part : (t + 1) * part], preferred_element_type=F32
        )
    for d in range(1, n_tp):
        t = turn(tp, d, n_tp)
        c = remote(dense_send.at[t], dense_recv.at[tp], de_s.at[d], de_r.at[d], me, t)
        c.start()
        dense.append(c)
    dense_recv[tp] = dense_send[tp]

    for i in (9, 10, 11):
        loads[i].wait()
    forwards = []
    for k in range(1, n_tp):
        c = remote(
            disp_recv.at[tp],
            disp_recv.at[turn(tp, n_tp - k, n_tp)],
            fw_s.at[k],
            fw_r.at[k],
            me,
            turn(tp, k, n_tp),
        )
        c.wait_recv()
        forwards.append(c)
    squares = jnp.zeros((slots, 1), F32)
    for t in range(n_tp):
        cols = pl.ds(t * part, part)
        for p in range(n_ep):
            rows_f[p * blk : (p + 1) * blk, cols] = disp_recv[t, p].astype(F32)
        x = rows_f[:, cols]
        squares += jnp.sum(x * x, axis=1, keepdims=True)
    inv = lax.rsqrt(squares / width + norm_eps)
    for t in range(n_tp):
        cols = pl.ds(t * part, part)
        rows_n[:, cols] = (rows_f[:, cols] * inv * gain[:, cols]).astype(BF16)
    x = rows_n[...]
    which = (lax.broadcasted_iota(jnp.int32, (slots, 1), 0) % blk) // CAP
    hidden = []
    for e in range(n_loc):
        h = silu(jnp.dot(x, eg[e], preferred_element_type=F32)) * jnp.dot(
            x, eu[e], preferred_element_type=F32
        )
        hidden.append(jnp.where(which == e, h, 0.0).astype(BF16))

    def down(t):
        cols = pl.ds(pl.multiple_of(t * part, 128), part)
        total = jnp.dot(hidden[0], ed[0, :, cols], preferred_element_type=F32)
        for e in range(1, n_loc):
            total += jnp.dot(hidden[e], ed[e, :, cols], preferred_element_type=F32)
        return total

    duo = []
    for y in range(n_row):
        pair_send[y] = down(y * CORES + (1 - core))
        c = remote(pair_send.at[y], pair_recv.at[y], pa_s.at[y], pa_r.at[y], me, partner)
        c.start()
        duo.append(c)
    for y in range(n_row):
        summed[y] = down(y * CORES + core)
    returns = []
    for y in range(n_row):
        duo[y].wait_recv()
        v = summed[y] + pair_recv[y]
        peak = jnp.max(jnp.abs(v), axis=1, keepdims=True)
        power = jnp.ceil(jnp.log(jnp.maximum(peak, 1e-30)) * LOG2E)
        coded[:, 0:part] = jnp.clip(
            jnp.floor(v * jnp.exp2(15.0 - power) + 0.5), -32767.0, 32767.0
        )
        coded[:, part : part + 128] = jnp.broadcast_to(power, (slots, 128))
        for p in range(n_ep):
            ret_send[y, p] = (
                coded[p * blk : (p + 1) * blk, :].astype(jnp.int32).astype(jnp.int16)
            )
    for d in range(1, n_ep):
        p = turn(me, d, n_ep)
        for k in range(n_row):
            y = turn(row, k, n_row)
            i = d * n_row + k
            c = remote(
                ret_send.at[y, p],
                ret_recv.at[row, me],
                re_s.at[i],
                re_r.at[i],
                p,
                y * CORES + core,
            )
            c.start()
            returns.append(c)
    for k in range(1, n_row):
        y = turn(row, k, n_row)
        c = remote(
            ret_send.at[y, me], ret_recv.at[row, me], re_s.at[k], re_r.at[k], me, y * CORES + core
        )
        c.start()
        returns.append(c)
    ret_recv[row, me] = ret_send[row, me]

    for c in dense:
        c.wait_recv()
    total = dense_recv[0]
    for t in range(1, n_tp):
        total += dense_recv[t]
    total = mix_gate * total
    for c in returns:
        c.wait_recv()
    mixed = jnp.zeros((slots, part), F32)
    for y in range(n_row):
        for p in range(n_ep):
            back[y, p * blk : (p + 1) * blk, :] = (
                ret_recv[y, p].astype(jnp.int32).astype(F32)
            )
        mixed += back[y, :, 0:part] * jnp.exp2(back[y, :, part : part + 1] - 15.0)
    total += jnp.dot(
        combine, mixed, preferred_element_type=F32, precision=lax.Precision.HIGHEST
    )
    sq_send[...] = jnp.broadcast_to(
        jnp.sum(total * total, axis=1, keepdims=True), sq_send.shape
    )
    swaps = []
    for d in range(1, n_tp):
        c = remote(sq_send, sq_recv.at[tp], sq_s.at[d], sq_r.at[d], me, turn(tp, d, n_tp))
        c.start()
        swaps.append(c)
    sq_recv[tp] = sq_send[...]
    for c in swaps:
        c.wait_recv()
    all_sq = sq_recv[0]
    for t in range(1, n_tp):
        all_sq += sq_recv[t]
    scale = lax.rsqrt(all_sq[:, 0:1] / width + norm_eps)
    out_ref[...] = (total * scale * og[...]).astype(out_ref.dtype)
    for c in gathers + list(sends.values()) + dense + forwards + duo + returns + swaps:
        c.wait_send()


def shards(n_ep, n_tp, *args):
    (tok, gain, route, logit, eg, eu, ed, dg, du, dd, mixw, og) = args
    t_rows, part = tok.shape
    width = part * n_tp
    n_loc, _, ff = eg.shape
    n_row = n_tp // CORES
    blk = n_loc * CAP
    slots = n_ep * blk
    dma = pltpu.SemaphoreType.DMA
    V = pltpu.VMEM
    scratch = [
        V((n_tp, t_rows, part), BF16),
        V((1, width), F32),
        V(route.shape[::-1], jnp.int32),
        V(logit.shape[::-1], F32),
        V(eg.shape, BF16),
        V(eu.shape, BF16),
        V(ed.shape, BF16),
        V(dg.shape, BF16),
        V(du.shape, BF16),
        V(dd.shape, BF16),
        V((1, width), F32),
        V((1, part), F32),
        V((t_rows, width), BF16),
        V((slots, part), F32),
        V((n_ep, blk, part), BF16),
        V((n_tp, n_ep, blk, part), BF16),
        V((slots, width), F32),
        V((slots, width), BF16),
        V((n_tp, t_rows, part), F32),
        V((n_tp, t_rows, part), F32),
        V((n_row, slots, part), F32),
        V((n_row, slots, part), F32),
        V((n_row, slots, part), F32),
        V((slots, part + 128), F32),
        V((n_row, n_ep, blk, part + 128), jnp.int16),
        V((n_row, n_ep, blk, part + 128), jnp.int16),
        V((n_row, slots, part + 128), F32),
        V((t_rows, 128), F32),
        V((n_tp, t_rows, 128), F32),
        dma((12,)),
        dma((n_tp,)),
        dma((n_tp,)),
        dma((n_ep,)),
        dma((n_ep,)),
        dma((n_tp,)),
        dma((n_tp,)),
        dma((n_tp,)),
        dma((n_tp,)),
        dma((n_row,)),
        dma((n_row,)),
        dma((n_ep * n_row,)),
        dma((n_ep * n_row,)),
        dma((n_tp,)),
        dma((n_tp,)),
    ]
    return pl.pallas_call(
        functools.partial(kernel, n_ep, n_tp),
        out_shape=jax.ShapeDtypeStruct((t_rows, part), BF16),
        in_specs=[pl.BlockSpec(memory_space=pltpu.HBM)] * 12,
        out_specs=pl.BlockSpec(memory_space=pltpu.VMEM),
        scratch_shapes=scratch,
        compiler_params=pltpu.CompilerParams(
            collective_id=0, has_side_effects=True, vmem_limit_bytes=60 * 1024 * 1024
        ),
        name="moe_layer",
    )(
        tok,
        gain.reshape(1, width),
        route.T,
        logit.T,
        eg,
        eu,
        ed,
        dg,
        du,
        dd,
        mixw.reshape(1, width),
        og.reshape(1, part),
    )


def solution(mesh):
    placed = (
        P("ep", "tp"),
        P(),
        P("ep", None),
        P("ep", None),
        P("ep", None, "tp"),
        P("ep", None, "tp"),
        P("ep", "tp", None),
        P(None, "tp"),
        P(None, "tp"),
        P("tp", None),
        P(),
        P("tp"),
    )
    return jax.shard_map(
        functools.partial(shards, mesh.shape["ep"], mesh.shape["tp"]),
        mesh=mesh,
        in_specs=placed,
        out_specs=P("ep", "tp"),
        check_vma=False,
    )
```

```python
import functools

import jax
import jax.numpy as jnp
from jax import lax
from jax.experimental import pallas as pl
from jax.experimental.pallas import tpu as pltpu
from jax.sharding import PartitionSpec as P

CAP = 2
CORES = 2
norm_eps = 1e-06
LOG2E = 1.4426950408889634
MESH = pl.DeviceIdType.MESH
F32 = jnp.float32
BF16 = jnp.bfloat16


def silu(v):
    return v / (1.0 + jnp.exp(-v))


def kernel(
    n_ep,
    n_tp,
    tok_hbm,
    gain_hbm,
    route_hbm,
    logit_hbm,
    eg_hbm,
    eu_hbm,
    ed_hbm,
    dg_hbm,
    du_hbm,
    dd_hbm,
    mix_hbm,
    og_hbm,
    out_ref,
    tok,
    gain,
    route,
    logit,
    eg,
    eu,
    ed,
    dg,
    du,
    dd,
    mixw,
    og,
    normed,
    placed,
    disp_send,
    disp_recv,
    rows_f,
    rows_n,
    dense_send,
    dense_recv,
    pair_send,
    pair_recv,
    summed,
    coded,
    ret_send,
    ret_recv,
    back,
    sq_send,
    sq_recv,
    lsem,
    ag_s,
    ag_r,
    di_s,
    di_r,
    fw_s,
    fw_r,
    de_s,
    de_r,
    pa_s,
    pa_r,
    re_s,
    re_r,
    sq_s,
    sq_r,
):
    me = lax.axis_index("ep")
    tp = lax.axis_index("tp")
    core = lax.rem(tp, CORES)
    row = lax.div(tp, CORES)
    n_row = n_tp // CORES
    partner = row * CORES + (1 - core)
    n_loc = eg.shape[0]
    t_rows, part = tok.shape[1], tok.shape[2]
    width = part * n_tp
    blk = n_loc * CAP
    slots = n_ep * blk

    def turn(base, d, n):
        return lax.rem(base + d, n)

    def remote(src, dst, s, r, e, t):
        return pltpu.make_async_remote_copy(
            src_ref=src,
            dst_ref=dst,
            send_sem=s,
            recv_sem=r,
            device_id={"ep": e, "tp": t},
            device_id_type=MESH,
        )

    barrier = pltpu.get_barrier_semaphore()
    greeted = 0
    for d in range(1, n_ep):
        pl.semaphore_signal(
            barrier, inc=1, device_id={"ep": turn(me, d, n_ep), "tp": tp}, device_id_type=MESH
        )
        greeted += 1
    for d in range(1, n_tp):
        pl.semaphore_signal(
            barrier, inc=1, device_id={"ep": me, "tp": turn(tp, d, n_tp)}, device_id_type=MESH
        )
        greeted += 1

    loads = []
    pairs = [
        (tok_hbm, tok.at[tp]),
        (gain_hbm, gain),
        (route_hbm, route),
        (logit_hbm, logit),
        (mix_hbm, mixw),
        (og_hbm, og),
        (dg_hbm, dg),
        (du_hbm, du),
        (dd_hbm, dd),
        (eg_hbm, eg),
        (eu_hbm, eu),
        (ed_hbm, ed),
    ]
    for i, (src, dst) in enumerate(pairs):
        c = pltpu.make_async_copy(src, dst, lsem.at[i])
        c.start()
        loads.append(c)

    near = sorted(range(1, n_ep), key=lambda d: min(d, n_ep - d))

    loads[0].wait()
    gathers = []
    for d in range(1, n_tp):
        gathers.append(
            remote(tok.at[tp], tok.at[tp], ag_s.at[d], ag_r.at[d], me, turn(tp, d, n_tp))
        )

    loads[2].wait()
    r0 = route[0:1, :]
    r1 = route[1:2, :]
    slot = lax.broadcasted_iota(jnp.int32, (slots, t_rows), 0)
    slot_e = slot // CAP
    slot_c = slot % CAP
    hit0 = (slot_e == r0).astype(F32)
    hit1 = (slot_e == r1).astype(F32)
    hits = hit0 + hit1
    ri = lax.broadcasted_iota(jnp.int32, (t_rows, t_rows), 0)
    ci = lax.broadcasted_iota(jnp.int32, (t_rows, t_rows), 1)
    before = jnp.dot(hits, (ri < ci).astype(F32), preferred_element_type=F32)
    place_t = hits * (before == slot_c.astype(F32)).astype(F32)

    placed[...] = jnp.dot(place_t.astype(BF16), tok[tp], preferred_element_type=F32)
    for p in range(n_ep):
        disp_send[p] = placed[p * blk : (p + 1) * blk, :].astype(BF16)
    for i in (1, 3, 4, 5):
        loads[i].wait()
    l0 = logit[0:1, :]
    l1 = logit[1:2, :]
    top = jnp.maximum(l0, l1)
    e0 = jnp.exp(l0 - top)
    e1 = jnp.exp(l1 - top)
    w0 = e0 / (e0 + e1)
    w1 = e1 / (e0 + e1)
    combine = (place_t * (hit0 * w0 + hit1 * w1)).T

    disp_recv[tp, me] = disp_send[me]

    pl.semaphore_wait(barrier, greeted)
    sends = {}
    for d in reversed(near):
        p = turn(me, d, n_ep)
        c = remote(disp_send.at[p], disp_recv.at[tp, me], di_s.at[d], di_r.at[d], p, tp)
        c.start()
        sends[d] = c
    for c in gathers:
        c.start()

    for d in [0] + near:
        q = turn(me, n_ep - d, n_ep)
        if d > 0:
            sends[d].wait_recv()
        for k in range(1, n_tp):
            remote(
                disp_recv.at[tp, q],
                disp_recv.at[tp, q],
                fw_s.at[k],
                fw_r.at[k],
                me,
                turn(tp, k, n_tp),
            ).start()

    for c in gathers:
        c.wait_recv()
    squares = jnp.zeros((t_rows, 1), F32)
    for t in range(n_tp):
        x = tok[t].astype(F32)
        squares += jnp.sum(x * x, axis=1, keepdims=True)
    inv = lax.rsqrt(squares / width + norm_eps)
    mix = jnp.zeros((t_rows, 1), F32)
    for t in range(n_tp):
        cols = pl.ds(t * part, part)
        nx = (tok[t].astype(F32) * inv * gain[:, cols]).astype(BF16)
        normed[:, cols] = nx
        mix += jnp.sum(nx.astype(F32) * mixw[:, cols], axis=1, keepdims=True)
    mix_gate = 1.0 / (1.0 + jnp.exp(-mix))

    for i in (6, 7):
        loads[i].wait()
    nrm = normed[...]
    dh = (
        silu(jnp.dot(nrm, dg[...], preferred_element_type=F32))
        * jnp.dot(nrm, du[...], preferred_element_type=F32)
    ).astype(BF16)
    for i in (8, 9, 10, 11):
        loads[i].wait()
    forwards = []
    for k in range(1, n_tp):
        c = remote(
            disp_recv.at[tp],
            disp_recv.at[turn(tp, n_tp - k, n_tp)],
            fw_s.at[k],
            fw_r.at[k],
            me,
            turn(tp, k, n_tp),
        )
        c.wait_recv()
        forwards.append(c)
    squares = jnp.zeros((slots, 1), F32)
    for t in range(n_tp):
        cols = pl.ds(t * part, part)
        for p in range(n_ep):
            rows_f[p * blk : (p + 1) * blk, cols] = disp_recv[t, p].astype(F32)
        x = rows_f[:, cols]
        squares += jnp.sum(x * x, axis=1, keepdims=True)
    inv = lax.rsqrt(squares / width + norm_eps)
    for t in range(n_tp):
        cols = pl.ds(t * part, part)
        rows_n[:, cols] = (rows_f[:, cols] * inv * gain[:, cols]).astype(BF16)
    x = rows_n[...]
    which = (lax.broadcasted_iota(jnp.int32, (slots, 1), 0) % blk) // CAP
    hidden = []
    for e in range(n_loc):
        h = silu(jnp.dot(x, eg[e], preferred_element_type=F32)) * jnp.dot(
            x, eu[e], preferred_element_type=F32
        )
        hidden.append(jnp.where(which == e, h, 0.0).astype(BF16))

    def down(t):
        cols = pl.ds(pl.multiple_of(t * part, 128), part)
        total = jnp.dot(hidden[0], ed[0, :, cols], preferred_element_type=F32)
        for e in range(1, n_loc):
            total += jnp.dot(hidden[e], ed[e, :, cols], preferred_element_type=F32)
        return total

    duo = []
    for y in range(n_row):
        pair_send[y] = down(y * CORES + (1 - core))
        c = remote(pair_send.at[y], pair_recv.at[y], pa_s.at[y], pa_r.at[y], me, partner)
        c.start()
        duo.append(c)
    for y in range(n_row):
        summed[y] = down(y * CORES + core)
    returns = []
    for y in range(n_row):
        duo[y].wait_recv()
        v = summed[y] + pair_recv[y]
        peak = jnp.max(jnp.abs(v), axis=1, keepdims=True)
        power = jnp.ceil(jnp.log(jnp.maximum(peak, 1e-30)) * LOG2E)
        coded[:, 0:part] = jnp.clip(
            jnp.floor(v * jnp.exp2(15.0 - power) + 0.5), -32767.0, 32767.0
        )
        coded[:, part : part + 128] = jnp.broadcast_to(power, (slots, 128))
        for p in range(n_ep):
            ret_send[y, p] = (
                coded[p * blk : (p + 1) * blk, :].astype(jnp.int32).astype(jnp.int16)
            )
    for d in range(1, n_ep):
        p = turn(me, d, n_ep)
        for k in range(n_row):
            y = turn(row, k, n_row)
            i = d * n_row + k
            c = remote(
                ret_send.at[y, p],
                ret_recv.at[row, me],
                re_s.at[i],
                re_r.at[i],
                p,
                y * CORES + core,
            )
            c.start()
            returns.append(c)
    for k in range(1, n_row):
        y = turn(row, k, n_row)
        c = remote(
            ret_send.at[y, me], ret_recv.at[row, me], re_s.at[k], re_r.at[k], me, y * CORES + core
        )
        c.start()
        returns.append(c)
    ret_recv[row, me] = ret_send[row, me]

    dense = []
    for t in range(n_tp):
        dense_send[t] = jnp.dot(
            dh, dd[:, t * part : (t + 1) * part], preferred_element_type=F32
        )
    for d in range(1, n_tp):
        t = turn(tp, d, n_tp)
        c = remote(dense_send.at[t], dense_recv.at[tp], de_s.at[d], de_r.at[d], me, t)
        c.start()
        dense.append(c)
    dense_recv[tp] = dense_send[tp]

    for c in dense:
        c.wait_recv()
    total = dense_recv[0]
    for t in range(1, n_tp):
        total += dense_recv[t]
    total = mix_gate * total
    for c in returns:
        c.wait_recv()
    mixed = jnp.zeros((slots, part), F32)
    for y in range(n_row):
        for p in range(n_ep):
            back[y, p * blk : (p + 1) * blk, :] = (
                ret_recv[y, p].astype(jnp.int32).astype(F32)
            )
        mixed += back[y, :, 0:part] * jnp.exp2(back[y, :, part : part + 1] - 15.0)
    total += jnp.dot(
        combine, mixed, preferred_element_type=F32, precision=lax.Precision.HIGHEST
    )
    sq_send[...] = jnp.broadcast_to(
        jnp.sum(total * total, axis=1, keepdims=True), sq_send.shape
    )
    swaps = []
    for d in range(1, n_tp):
        c = remote(sq_send, sq_recv.at[tp], sq_s.at[d], sq_r.at[d], me, turn(tp, d, n_tp))
        c.start()
        swaps.append(c)
    sq_recv[tp] = sq_send[...]
    for c in swaps:
        c.wait_recv()
    all_sq = sq_recv[0]
    for t in range(1, n_tp):
        all_sq += sq_recv[t]
    scale = lax.rsqrt(all_sq[:, 0:1] / width + norm_eps)
    out_ref[...] = (total * scale * og[...]).astype(out_ref.dtype)
    for c in gathers + list(sends.values()) + dense + forwards + duo + returns + swaps:
        c.wait_send()


def shards(n_ep, n_tp, *args):
    (tok, gain, route, logit, eg, eu, ed, dg, du, dd, mixw, og) = args
    t_rows, part = tok.shape
    width = part * n_tp
    n_loc, _, ff = eg.shape
    n_row = n_tp // CORES
    blk = n_loc * CAP
    slots = n_ep * blk
    dma = pltpu.SemaphoreType.DMA
    V = pltpu.VMEM
    scratch = [
        V((n_tp, t_rows, part), BF16),
        V((1, width), F32),
        V(route.shape[::-1], jnp.int32),
        V(logit.shape[::-1], F32),
        V(eg.shape, BF16),
        V(eu.shape, BF16),
        V(ed.shape, BF16),
        V(dg.shape, BF16),
        V(du.shape, BF16),
        V(dd.shape, BF16),
        V((1, width), F32),
        V((1, part), F32),
        V((t_rows, width), BF16),
        V((slots, part), F32),
        V((n_ep, blk, part), BF16),
        V((n_tp, n_ep, blk, part), BF16),
        V((slots, width), F32),
        V((slots, width), BF16),
        V((n_tp, t_rows, part), F32),
        V((n_tp, t_rows, part), F32),
        V((n_row, slots, part), F32),
        V((n_row, slots, part), F32),
        V((n_row, slots, part), F32),
        V((slots, part + 128), F32),
        V((n_row, n_ep, blk, part + 128), jnp.int16),
        V((n_row, n_ep, blk, part + 128), jnp.int16),
        V((n_row, slots, part + 128), F32),
        V((t_rows, 128), F32),
        V((n_tp, t_rows, 128), F32),
        dma((12,)),
        dma((n_tp,)),
        dma((n_tp,)),
        dma((n_ep,)),
        dma((n_ep,)),
        dma((n_tp,)),
        dma((n_tp,)),
        dma((n_tp,)),
        dma((n_tp,)),
        dma((n_row,)),
        dma((n_row,)),
        dma((n_ep * n_row,)),
        dma((n_ep * n_row,)),
        dma((n_tp,)),
        dma((n_tp,)),
    ]
    return pl.pallas_call(
        functools.partial(kernel, n_ep, n_tp),
        out_shape=jax.ShapeDtypeStruct((t_rows, part), BF16),
        in_specs=[pl.BlockSpec(memory_space=pltpu.HBM)] * 12,
        out_specs=pl.BlockSpec(memory_space=pltpu.VMEM),
        scratch_shapes=scratch,
        compiler_params=pltpu.CompilerParams(
            collective_id=0, has_side_effects=True, vmem_limit_bytes=60 * 1024 * 1024
        ),
        name="moe_layer",
    )(
        tok,
        gain.reshape(1, width),
        route.T,
        logit.T,
        eg,
        eu,
        ed,
        dg,
        du,
        dd,
        mixw.reshape(1, width),
        og.reshape(1, part),
    )


def solution(mesh):
    placed = (
        P("ep", "tp"),
        P(),
        P("ep", None),
        P("ep", None),
        P("ep", None, "tp"),
        P("ep", None, "tp"),
        P("ep", "tp", None),
        P(None, "tp"),
        P(None, "tp"),
        P("tp", None),
        P(),
        P("tp"),
    )
    return jax.shard_map(
        functools.partial(shards, mesh.shape["ep"], mesh.shape["tp"]),
        mesh=mesh,
        in_specs=placed,
        out_specs=P("ep", "tp"),
        check_vma=False,
    )
```
